32 devices in a mesh: grp: 2 (over y), sp: 4 (over z), tp: 4 (over x, core).
Axes of the slice: x: 2, y: 2, z: 4, core: 2. Of those that a mesh axis runs over, the one named last changes fastest.
Arguments:
- tokens: bfloat16 [3072, 2048], P(('grp', 'sp'), 'tp'), parts along dimension 0, may hold values from -6 to 6
- norm_gain: float32 [2048], replicated, may hold values from 0.1 to 1.9
- qk_gain: float32 [4, 64], replicated, may hold values from 0.7 to 5.5
- w_query_window: bfloat16 [2048, 1024], P('sp', 'tp'), may hold values from -1 to 1
- w_key_window: bfloat16 [2048, 512], P('sp', 'tp'), may hold values from -1 to 1
- w_value_window: bfloat16 [2048, 512], P('sp', 'tp'), may hold values from -0.125 to 0.125
- sink_logits: float32 [16], P('tp'), may hold values from 0 to 5
- w_query_forget: bfloat16 [2048, 1024], P('sp', 'tp'), may hold values from -1 to 1
- w_key_forget: bfloat16 [2048, 1024], P('sp', 'tp'), may hold values from -1 to 1
- w_value_forget: bfloat16 [2048, 1024], P('sp', 'tp'), may hold values from -0.125 to 0.125
- gate_cum: float32 [3072, 16], P(('grp', 'sp'), 'tp'), parts along dimension 0, as said below
- w_merge: bfloat16 [2048, 2, 2048], P('sp', None, 'tp'), may hold values from -0.125 to 0.125
- w_branch: bfloat16 [2, 1024, 2048], P(None, 'sp', 'tp'), may hold values from -0.8984375 to 0.8984375
Outputs:
- mixed: bfloat16 [3072, 2048], P(('grp', 'sp'), 'tp'), parts along dimension 0
The draws below stay inside these ranges and needn't reach their ends.
There are 2 independent parts, one for each index of `grp`. The reference program is written for one: setup_inputs(seed, part) draws one part's arguments, and reference() takes and returns one part's arrays. A program takes and returns all parts, laid end to end along the dimension named above; an argument that names none is the same for every part. Nothing has to cross between parts.
Inputs may be any that keep to these rules, and one draw needn't show every extreme that they name: `gate_cum`: along positions each head's values never rise.
All inputs are finite; a program needn't handle non-finite values.
Results may differ from the reference program's by a relative error of at most 0.012.
Values may be sent and summed in bfloat16 or wider, within the bound.
A program may use at most 64 MiB of HBM per device.

```python
import math
import jax
import jax.numpy as jnp
from jax import lax

D = 2048
QUERY_HEAD_COUNT = 16
KV_HEADS = 8
HEAD = 64
WINDOW = 128
TOK_DEV = 384
SEQUENCE_LENGTH = 1536


def query_raw(key, offset_salt, col_count):
    return jax.random.normal(jax.random.fold_in(key, offset_salt), (D, col_count), jnp.float32) * D ** (-0.5)


def draw_qk_gain(key, part):
    gain_table = jax.random.uniform(jax.random.fold_in(key, 7), (4, HEAD), jnp.float32, 0.7, 1.3)
    return gain_table


def draw_w_query_window(key, part):
    return query_raw(key, 11, QUERY_HEAD_COUNT * HEAD).astype(jnp.bfloat16)


def draw_w_key_window(key, part):
    fresh_part = query_raw(key, 12, KV_HEADS * HEAD)
    return fresh_part.astype(jnp.bfloat16)


def draw_w_query_forget(key, part):
    return query_raw(key, 13, QUERY_HEAD_COUNT * HEAD).astype(jnp.bfloat16)


def draw_w_key_forget(key, part):
    fresh_part = query_raw(key, 14, QUERY_HEAD_COUNT * HEAD)
    return fresh_part.astype(jnp.bfloat16)


def draw_gate_cum(key, part):
    head_order = jax.random.permutation(jax.random.fold_in(key, 21), QUERY_HEAD_COUNT)
    lagging_heads = head_order < QUERY_HEAD_COUNT // 2
    slow_rate = jnp.exp(jax.random.uniform(jax.random.fold_in(key, 22), (QUERY_HEAD_COUNT,), jnp.float32, jnp.log(0.3), jnp.log(1.2))) / SEQUENCE_LENGTH
    fast_rate = jnp.exp(jax.random.uniform(jax.random.fold_in(key, 23), (QUERY_HEAD_COUNT,), jnp.float32, jnp.log(0.01), jnp.log(0.033)))
    step_rate = jnp.where(lagging_heads, slow_rate, fast_rate)
    block_factor = jnp.exp(jax.random.uniform(jax.random.fold_in(key, 24), (SEQUENCE_LENGTH // TOK_DEV, QUERY_HEAD_COUNT), jnp.float32, jnp.log(0.5), jnp.log(2.0)))
    block_factor = jnp.repeat(block_factor, TOK_DEV, axis=0)
    jitter = jax.random.uniform(jax.random.fold_in(key, 25), (SEQUENCE_LENGTH, QUERY_HEAD_COUNT), jnp.float32, 0.3, 1.7)
    step_count = -step_rate[None, :] * block_factor * jitter
    spike_locations = jax.random.randint(jax.random.fold_in(key, 26), (3,), 0, SEQUENCE_LENGTH)
    spike_misses = jnp.log(1.0 - jax.random.uniform(jax.random.fold_in(key, 27), (3, QUERY_HEAD_COUNT), jnp.float32, 0.2, 0.4))
    spike_matches = (jnp.arange(SEQUENCE_LENGTH)[:, None] == spike_locations[None, :]).astype(jnp.float32)
    spike_events = jnp.dot(spike_matches, spike_misses) * lagging_heads.astype(jnp.float32)[None, :]
    return jnp.cumsum(step_count + spike_events, axis=0)


def block_scale(own_key, shape, cuts, least, high):
    level = 1.0
    for position, shards_of in cuts:
        steps = jax.random.uniform(jax.random.fold_in(jax.random.fold_in(own_key, 6), position), (shards_of,), jnp.float32, least / len(cuts), high / len(cuts))
        level = level * jnp.repeat(jnp.exp(steps), shape[position] // shards_of).reshape((-1,) + (1,) * (len(shape) - 1 - position))
    return level


def scatter_about(own_key, dims, deviation, bound, cuts=(), kind=jnp.bfloat16):
    level = block_scale(own_key, dims, cuts, -0.22, 0.18) if cuts else 1.0
    array = jax.random.normal(own_key, dims, jnp.float32) * deviation * level
    return jnp.minimum(jnp.maximum(array, -bound), bound).astype(kind)


def setup_inputs(seed: int = 0, part: int = 0) -> dict:
    arg_keys = jax.random.split(jax.random.key(seed), 14)
    own_keys = jax.random.split(jax.random.fold_in(arg_keys[13], part), 14)
    tokens = scatter_about(own_keys[0], (SEQUENCE_LENGTH, D), 1.0, 6.0, ((0, 4), (1, 4)))
    norm_gain = jnp.clip(1.0 + 0.18 * jax.random.normal(arg_keys[1], (D,), jnp.float32), 0.1, 1.9)
    qk_gain = draw_qk_gain(jax.random.fold_in(arg_keys[13], 71), part)
    w_query_window = draw_w_query_window(jax.random.fold_in(arg_keys[13], 71), part)
    w_key_window = draw_w_key_window(jax.random.fold_in(arg_keys[13], 71), part)
    w_value_window = scatter_about(arg_keys[5], (D, KV_HEADS * HEAD), D ** -0.5, 0.125, ((0, 4), (1, 4)))
    sink_logits = jnp.clip(5.0 * jax.random.uniform(arg_keys[6], (QUERY_HEAD_COUNT,), jnp.float32) ** block_scale(arg_keys[6], (QUERY_HEAD_COUNT,), ((0, 4),), -0.2, 0.2), 0.0, 5.0)
    w_query_forget = draw_w_query_forget(jax.random.fold_in(arg_keys[13], 71), part)
    w_key_forget = draw_w_key_forget(jax.random.fold_in(arg_keys[13], 71), part)
    w_value_forget = scatter_about(arg_keys[9], (D, QUERY_HEAD_COUNT * HEAD), D ** -0.5, 0.125, ((0, 4), (1, 4)))
    gate_cum = draw_gate_cum(jax.random.fold_in(jax.random.fold_in(arg_keys[13], part), 71), part)
    w_merge = scatter_about(arg_keys[11], (D, 2, D), D ** -0.5, 0.125, ((0, 4), (2, 4)))
    w_branch = scatter_about(arg_keys[12], (2, QUERY_HEAD_COUNT * HEAD, D), 0.15, 0.8984375, ((1, 4), (2, 4)))
    return {"tokens": tokens, "norm_gain": norm_gain, "qk_gain": qk_gain, "w_query_window": w_query_window, "w_key_window": w_key_window, "w_value_window": w_value_window, "sink_logits": sink_logits, "w_query_forget": w_query_forget, "w_key_forget": w_key_forget, "w_value_forget": w_value_forget, "gate_cum": gate_cum, "w_merge": w_merge, "w_branch": w_branch}


epsilon = 1e-06
big_negative = -1e+30

def rounded(value):
    return lax.optimization_barrier(value.astype(jnp.bfloat16)).astype(jnp.float32)

def head_norm(raw, gain, head_count):
    split = raw.reshape(raw.shape[0], head_count, -1)
    scaled = split * lax.rsqrt(lax.optimization_barrier(jnp.mean(split * split, axis=-1, keepdims=True)) + epsilon) * gain
    return scaled.astype(jnp.bfloat16)

def window_attend(queries, keys_ext, values_ext, sink_rows, first_pos):
    row_count, head_count, head_size = queries.shape
    group_count = keys_ext.shape[1]
    span_rows = WINDOW // 2
    block_count = row_count // span_rows
    query_blocks = queries.reshape(block_count, span_rows, group_count, head_count // group_count, head_size).astype(jnp.float32)
    key_blocks = jnp.concatenate([keys_ext[lag_index * span_rows:lag_index * span_rows + row_count].reshape(block_count, span_rows, group_count, head_size) for lag_index in range(3)], axis=1).astype(jnp.float32)
    value_blocks = jnp.concatenate([values_ext[lag_index * span_rows:lag_index * span_rows + row_count].reshape(block_count, span_rows, group_count, head_size) for lag_index in range(3)], axis=1).astype(jnp.float32)
    scores = jnp.einsum('nqgrd,nkgd->ngrqk', query_blocks, key_blocks) * head_size ** (-0.5)
    distance = WINDOW + jnp.arange(span_rows)[:, None] - jnp.arange(3 * span_rows)[None, :]
    key_pos = first_pos - WINDOW + jnp.arange(block_count)[:, None] * span_rows + jnp.arange(3 * span_rows)[None, :]
    is_valid = ((distance >= 0) & (distance < WINDOW))[None] & (key_pos >= 0)[:, None, :]
    is_valid = is_valid[:, None, None]
    sink_grid = sink_rows.reshape(1, group_count, head_count // group_count, 1)
    row_max = jnp.maximum(lax.optimization_barrier(jnp.max(jnp.where(is_valid, scores, big_negative), axis=-1)), sink_grid)
    weights = jnp.where(is_valid, jnp.exp(scores - row_max[..., None]), 0.0)
    row_total = lax.optimization_barrier(jnp.sum(weights, axis=-1)) + jnp.exp(sink_grid - row_max)
    prob_rows = rounded(weights / row_total[..., None])
    mixed_sum = jnp.einsum('ngrqk,nkgd->nqgrd', prob_rows, value_blocks)
    return mixed_sum.reshape(row_count, head_count * head_size).astype(jnp.bfloat16)

def forget_attend(queries, keys, values, gates):
    row_count, head_count, head_size = queries.shape
    block_rows = math.gcd(row_count, 512)
    block_count = row_count // block_rows
    key_float = keys.astype(jnp.float32)
    value_float = values.astype(jnp.float32)
    key_pos = jnp.arange(row_count)

    def one_block(inputs):
        block_index, query_block, gate_block = inputs
        scores = jnp.einsum('qhd,khd->hqk', query_block.astype(jnp.float32), key_float) * head_size ** (-0.5)
        scores = scores + gate_block.T[:, :, None] - gates.T[:, None, :]
        query_pos = block_index * block_rows + jnp.arange(block_rows)
        is_valid = (query_pos[:, None] >= key_pos[None, :])[None]
        scores = jnp.where(is_valid, scores, big_negative)
        row_max = lax.optimization_barrier(jnp.max(scores, axis=-1))
        weights = jnp.where(is_valid, jnp.exp(scores - row_max[..., None]), 0.0)
        row_total = lax.optimization_barrier(jnp.sum(weights, axis=-1))
        mixed_sum = jnp.einsum('hqk,khd->qhd', rounded(weights), value_float)
        return mixed_sum / row_total.T[:, :, None]
    result = lax.map(one_block, (jnp.arange(block_count), queries.reshape(block_count, block_rows, head_count, head_size), gates.reshape(block_count, block_rows, head_count)))
    return result.reshape(row_count, head_count * head_size).astype(jnp.bfloat16)

def reference(tokens, norm_gain, qk_gain, w_query_window, w_key_window, w_value_window, sink_logits, w_query_forget, w_key_forget, w_value_forget, gate_cum, w_merge, w_branch):
    as_float = tokens.astype(jnp.float32)
    normed = (as_float * lax.rsqrt(lax.optimization_barrier(jnp.mean(as_float * as_float, axis=-1, keepdims=True)) + epsilon) * norm_gain).astype(jnp.bfloat16)

    def project(weight):
        return jnp.dot(normed, weight, preferred_element_type=jnp.float32)
    window_query = head_norm(project(w_query_window), qk_gain[0], QUERY_HEAD_COUNT)
    window_key = head_norm(project(w_key_window), qk_gain[1], KV_HEADS)
    window_value = project(w_value_window).astype(jnp.bfloat16).reshape(SEQUENCE_LENGTH, KV_HEADS, HEAD)
    padding = jnp.zeros((WINDOW, KV_HEADS, HEAD), jnp.bfloat16)
    window_out = window_attend(window_query, jnp.concatenate([padding, window_key], axis=0), jnp.concatenate([padding, window_value], axis=0), sink_logits, 0)
    forget_query = head_norm(project(w_query_forget), qk_gain[2], QUERY_HEAD_COUNT)
    forget_key = head_norm(project(w_key_forget), qk_gain[3], QUERY_HEAD_COUNT)
    forget_value = project(w_value_forget).astype(jnp.bfloat16).reshape(SEQUENCE_LENGTH, QUERY_HEAD_COUNT, HEAD)
    forget_out = forget_attend(forget_query, forget_key, forget_value, gate_cum)
    merge_gate = jax.nn.sigmoid(project(w_merge.reshape(D, 2 * D))).reshape(SEQUENCE_LENGTH, 2, D)
    window_projection = jnp.dot(window_out, w_branch[0], preferred_element_type=jnp.float32)
    forget_projection = jnp.dot(forget_out, w_branch[1], preferred_element_type=jnp.float32)
    return (merge_gate[:, 0] * window_projection + merge_gate[:, 1] * forget_projection).astype(jnp.bfloat16)
```

```python
import functools

import jax
import jax.numpy as jnp
from jax import lax
from jax.experimental import pallas as pl
from jax.experimental.pallas import tpu as pltpu
from jax.sharding import PartitionSpec as P

HEAD = 64
PAIR = 2 * HEAD
WINDOW = 128

epsilon = 1e-06
big_negative = -1e30
VMEM_LIMIT = 60 * 1024 * 1024


def from_behind(value, axis, by):
    size = lax.axis_size(axis)
    pairs = [(i, i + by) for i in range(size) if 0 <= i + by < size]
    return lax.ppermute(value, axis, pairs)


def project_kernel(sections, tokens_ref, gain_ref, weight_ref, head_gain_ref, normed_ref, *outs):
    x = tokens_ref[...].astype(jnp.float32)
    scale = lax.rsqrt(jnp.mean(x * x, axis=-1, keepdims=True) + epsilon)
    normed_ref[...] = (x * scale * gain_ref[...]).astype(jnp.bfloat16)
    low = lax.broadcasted_iota(jnp.int32, (1, PAIR), 1) < HEAD
    normed = normed_ref[...]
    start = 0
    for out_ref, flags in zip(outs, sections):
        width = out_ref.shape[1]
        raw = jnp.dot(normed, weight_ref[:, start : start + width], preferred_element_type=jnp.float32)
        for at in range(0, width, PAIR):
            part = raw[:, at : at + PAIR]
            first, second = flags[at // HEAD], flags[at // HEAD + 1]
            if first or second:
                squares = part * part
                lower = jnp.sum(jnp.where(low, squares, 0.0), axis=-1, keepdims=True)
                upper = jnp.sum(jnp.where(low, 0.0, squares), axis=-1, keepdims=True)
                factor = jnp.where(
                    low,
                    lax.rsqrt(lower * (1.0 / HEAD) + epsilon),
                    lax.rsqrt(upper * (1.0 / HEAD) + epsilon),
                )
                scaled = part * factor * head_gain_ref[:, start + at : start + at + PAIR]
                if first and second:
                    part = scaled
                else:
                    part = jnp.where(low if first else ~low, scaled, part)
            out_ref[:, at : at + PAIR] = part.astype(jnp.bfloat16)
        start += width


def attend_kernel(heads, q_ref, kv_ref, gates_ref, wkv_ref, sink_ref, out_ref):
    rows = q_ref.shape[0]
    width = heads * HEAD
    shard = lax.axis_index("sp")
    low = lax.broadcasted_iota(jnp.int32, (1, PAIR), 1) < HEAD
    contract = (((1,), (1,)), ((), ()))
    for pair in range(heads // 2):
        lanes = pair * PAIR
        queries = q_ref[:, width + lanes : width + lanes + PAIR] * jnp.bfloat16(HEAD ** -0.5)
        split = [jnp.where(low, queries, jnp.bfloat16(0)), jnp.where(low, jnp.bfloat16(0), queries)]
        diagonal = lax.broadcasted_iota(jnp.int32, (rows, rows), 0) >= lax.broadcasted_iota(
            jnp.int32, (rows, rows), 1
        )

        def block(index, carry, masked):
            at = pl.ds(pl.multiple_of(index * rows, rows), rows)
            keys = kv_ref[at, lanes : lanes + PAIR]
            values = kv_ref[at, width + lanes : width + lanes + PAIR]
            result = []
            for half in range(2):
                top, total, mixed = carry[half]
                head = pair * 2 + half
                scores = lax.dot_general(split[half], keys, contract, preferred_element_type=jnp.float32)
                scores = scores - gates_ref[index, head : head + 1, :]
                if masked:
                    scores = jnp.where(diagonal, scores, big_negative)
                new_top = jnp.maximum(top, jnp.max(scores, axis=-1, keepdims=True))
                weights = jnp.exp(scores - new_top)
                if masked:
                    weights = jnp.where(diagonal, weights, 0.0)
                shrink = jnp.exp(top - new_top)
                total = total * shrink + jnp.sum(weights, axis=-1, keepdims=True)
                mixed = mixed * shrink + jnp.dot(
                    weights.astype(jnp.bfloat16), values, preferred_element_type=jnp.float32
                )
                result.append((new_top, total, mixed))
            return tuple(result)

        empty = (
            jnp.full((rows, 1), big_negative, jnp.float32),
            jnp.zeros((rows, 1), jnp.float32),
            jnp.zeros((rows, PAIR), jnp.float32),
        )
        state = block(shard, (empty, empty), True)
        state = lax.fori_loop(0, shard, lambda i, c: block(i, c, False), state)
        mixed = jnp.where(low, state[0][2] / state[0][1], state[1][2] / state[1][1])
        out_ref[:, width + lanes : width + lanes + PAIR] = mixed.astype(jnp.bfloat16)

        keys = wkv_ref[:, pair * HEAD : (pair + 1) * HEAD]
        values = wkv_ref[:, width // 2 + pair * HEAD : width // 2 + (pair + 1) * HEAD]
        keys = jnp.concatenate([keys, keys], axis=1)
        values = jnp.concatenate([values, values], axis=1)
        row_at = lax.broadcasted_iota(jnp.int32, (WINDOW, 2 * WINDOW), 0)
        col_at = lax.broadcasted_iota(jnp.int32, (WINDOW, 2 * WINDOW), 1)
        inside = (col_at > row_at) & (col_at <= row_at + WINDOW)
        for at in range(0, rows, WINDOW):
            queries = q_ref[at : at + WINDOW, lanes : lanes + PAIR] * jnp.bfloat16(HEAD ** -0.5)
            near = keys[at : at + 2 * WINDOW]
            near_values = values[at : at + 2 * WINDOW]
            valid = inside
            if at == 0:
                valid = inside & ((col_at >= WINDOW) | (shard > 0))
            parts = []
            for half in range(2):
                head = pair * 2 + half
                mine = jnp.where(low if half == 0 else ~low, queries, jnp.bfloat16(0))
                scores = lax.dot_general(mine, near, contract, preferred_element_type=jnp.float32)
                sink = sink_ref[:, head : head + 1]
                top = jnp.maximum(
                    jnp.max(jnp.where(valid, scores, big_negative), axis=-1, keepdims=True), sink
                )
                weights = jnp.where(valid, jnp.exp(scores - top), 0.0)
                total = jnp.sum(weights, axis=-1, keepdims=True) + jnp.exp(sink - top)
                probs = (weights / total).astype(jnp.bfloat16)
                parts.append(jnp.dot(probs, near_values, preferred_element_type=jnp.float32))
            out_ref[at : at + WINDOW, lanes : lanes + PAIR] = jnp.where(low, parts[0], parts[1]).astype(
                jnp.bfloat16
            )


def gather_rows(shard):
    parts = lax.axis_size("grp")
    rows = shard.shape[0] // parts
    mine = lax.dynamic_slice_in_dim(shard, lax.axis_index("grp") * rows, rows, axis=0)
    return lax.all_gather(mine, ("sp", "grp"), axis=0, tiled=True)


def on_device(
    tokens,
    norm_gain,
    qk_gain,
    w_query_window,
    w_key_window,
    w_value_window,
    sink_logits,
    w_query_forget,
    w_key_forget,
    w_value_forget,
    gate_cum,
    w_merge,
    w_branch,
):
    rows = tokens.shape[0]
    shards = lax.axis_size("sp")
    heads = w_query_window.shape[1] // HEAD
    groups = w_key_window.shape[1] // HEAD
    channels = w_merge.shape[2]
    gathered = lax.all_gather(tokens, "tp", axis=1, tiled=True)
    weights = gather_rows(
        jnp.concatenate(
            [w_query_window, w_query_forget, w_key_forget, w_value_forget, w_key_window, w_value_window],
            axis=1,
        )
    )
    head_gains = jnp.concatenate(
        [
            jnp.tile(qk_gain[0], heads),
            jnp.tile(qk_gain[2], heads),
            jnp.tile(qk_gain[3], heads),
            jnp.ones((heads * HEAD,), jnp.float32),
            jnp.tile(qk_gain[1], groups),
            jnp.ones((groups * HEAD,), jnp.float32),
        ]
    )[None]
    sections = (
        (True,) * (2 * heads),
        (True,) * heads + (False,) * heads,
        (True,) * groups + (False,) * groups,
    )
    depth = gathered.shape[1]
    normed, queries, forget_kv, window_kv = pl.pallas_call(
        functools.partial(project_kernel, sections),
        out_shape=(
            jax.ShapeDtypeStruct((rows, depth), jnp.bfloat16),
            *(jax.ShapeDtypeStruct((rows, len(s) * HEAD), jnp.bfloat16) for s in sections),
        ),
        compiler_params=pltpu.CompilerParams(vmem_limit_bytes=VMEM_LIMIT),
        cost_estimate=pl.CostEstimate(
            flops=2 * rows * depth * weights.shape[1], bytes_accessed=8 * 1024 * 1024, transcendentals=0
        ),
        name="project",
    )(gathered, norm_gain[None], weights, head_gains)
    behind = from_behind(window_kv[rows - WINDOW :], "sp", 1)
    kv_all = lax.all_gather(forget_kv, "sp", axis=0, tiled=True)
    gates_all = lax.all_gather(gate_cum.T, "sp", axis=0)
    attended = pl.pallas_call(
        functools.partial(attend_kernel, heads),
        out_shape=jax.ShapeDtypeStruct((rows, 2 * heads * HEAD), jnp.bfloat16),
        compiler_params=pltpu.CompilerParams(vmem_limit_bytes=VMEM_LIMIT),
        cost_estimate=pl.CostEstimate(
            flops=8 * rows * rows * shards * heads * HEAD,
            bytes_accessed=4 * 1024 * 1024,
            transcendentals=rows * rows * shards * heads,
        ),
        name="attend",
    )(queries, kv_all, gates_all, jnp.concatenate([behind, window_kv], axis=0), sink_logits[None])
    merge_rows = gather_rows(w_merge.reshape(w_merge.shape[0], -1))
    merge_gate = jax.nn.sigmoid(jnp.dot(normed, merge_rows, preferred_element_type=jnp.float32))
    branch_full = gather_rows(w_branch.swapaxes(0, 1)).swapaxes(0, 1)
    width = heads * HEAD
    head_all = lax.all_gather(attended.reshape(rows, 2, width), "tp", axis=2, tiled=True)
    window_projection = jnp.dot(head_all[:, 0], branch_full[0], preferred_element_type=jnp.float32)
    forget_projection = jnp.dot(head_all[:, 1], branch_full[1], preferred_element_type=jnp.float32)
    return (
        merge_gate[:, :channels] * window_projection + merge_gate[:, channels:] * forget_projection
    ).astype(jnp.bfloat16)


def solution(mesh):
    return jax.shard_map(
        on_device,
        mesh=mesh,
        in_specs=(
            P(("grp", "sp"), "tp"),
            P(),
            P(),
            P("sp", "tp"),
            P("sp", "tp"),
            P("sp", "tp"),
            P("tp"),
            P("sp", "tp"),
            P("sp", "tp"),
            P("sp", "tp"),
            P(("grp", "sp"), "tp"),
            P("sp", None, "tp"),
            P(None, "sp", "tp"),
        ),
        out_specs=P(("grp", "sp"), "tp"),
        check_vma=False,
    )
```

```python
import functools

import jax
import jax.numpy as jnp
from jax import lax
from jax.experimental import pallas as pl
from jax.experimental.pallas import tpu as pltpu
from jax.sharding import PartitionSpec as P

HEAD = 64
PAIR = 2 * HEAD
WINDOW = 128

epsilon = 1e-06
big_negative = -1e30
MESH = pl.DeviceIdType.MESH
VMEM_LIMIT = 60 * 1024 * 1024


def layer_kernel(
    heads, groups,
    tokens_in, kv_in, q_in, merge_in, branch_in, gates_in, norm_gain, head_gain, sink_ref,
    out_ref,
    tok, normed, w_kv, w_q, w_m0, w_m1, w_br, kv, gates, wkv, queries, win, forg, top_s, total_s, mixed_s, gate_s,
    local_sem, tok_sem, z_send, z_recv, y_send, y_recv, kv_send, kv_recv, gt_send, gt_recv, halo_sem, head_sem,
):
    shards, parts, ways = lax.axis_size("sp"), lax.axis_size("grp"), lax.axis_size("tp")
    s, g, t = lax.axis_index("sp"), lax.axis_index("grp"), lax.axis_index("tp")
    rows, depth = normed.shape
    width = heads * HEAD
    low = lax.broadcasted_iota(jnp.int32, (1, PAIR), 1) < HEAD
    contract = (((1,), (1,)), ((), ()))

    chunks = [w_kv, w_q, w_m0, w_m1, w_br]

    def view(chunk, block, part=None):
        ref = chunks[chunk]
        axis = ref.ndim - 2
        share = ref.shape[axis] // shards
        start, size = block * share, share
        if part is not None:
            size = share // parts
            start = start + part * size
        at = pl.ds(pl.multiple_of(start, size), size)
        return ref.at[at, :] if axis == 0 else ref.at[:, at, :]

    def z_copy(direction, chunk, block, index):
        return pltpu.make_async_remote_copy(
            src_ref=view(chunk, block, g),
            dst_ref=view(chunk, block, g),
            send_sem=z_send.at[direction, chunk, index],
            recv_sem=z_recv.at[direction, chunk, index],
            device_id={"sp": s + 1 if direction == 0 else s - 1},
            device_id_type=MESH,
        )

    def y_copy(direction, chunk, block, index, shift, part):
        return pltpu.make_async_remote_copy(
            src_ref=view(chunk, block, part),
            dst_ref=view(chunk, block, part),
            send_sem=y_send.at[direction, chunk, index, shift - 1],
            recv_sem=y_recv.at[direction, chunk, index, shift - 1],
            device_id={"grp": lax.rem(g + shift, parts)},
            device_id_type=MESH,
        )

    def has_next(direction):
        return s + 1 < shards if direction == 0 else s > 0

    def source(direction, step):
        return s - step if direction == 0 else s + step

    def has_source(direction, step):
        return s >= step if direction == 0 else s + step < shards

    def send_own(chunk):
        for direction in range(2):
            @pl.when(has_next(direction))
            def _():
                z_copy(direction, chunk, s, 0).start()

    def relay(chunk, step):
        for direction in range(2):
            @pl.when(has_source(direction, step))
            def _():
                block = source(direction, step)
                z_copy(direction, chunk, block, step - 1).wait_recv()

                @pl.when(has_next(direction) & (step < shards - 1))
                def _():
                    z_copy(direction, chunk, block, step).start()

                for shift in range(1, parts):
                    y_copy(direction, chunk, block, step - 1, shift, g).start()

    def wait_mirror(chunk):
        @pl.loop(1, shards)
        def _(step):
            for direction in range(2):
                @pl.when(has_source(direction, step))
                def _():
                    for shift in range(1, parts):
                        part = lax.rem(g + parts - shift, parts)
                        y_copy(direction, chunk, source(direction, step), step - 1, shift, part).wait_recv()

    def local(index, src, dst):
        return pltpu.make_async_copy(src, dst, local_sem.at[index])

    locals_ = []
    for index, (array, chunk) in enumerate(((kv_in, 0), (q_in, 1))):
        locals_.append(local(index, array, view(chunk, s)))
    channels = out_ref.shape[1]
    locals_.append(local(2, tokens_in, tok.at[t]))
    locals_.append(local(3, gates_in, gates.at[s]))
    locals_.append(local(4, merge_in.at[:, 0:channels], view(2, s)))
    locals_.append(local(5, merge_in.at[:, channels : 2 * channels], view(3, s)))
    locals_.append(local(6, branch_in, view(4, s)))
    for copy in locals_:
        copy.start()

    barrier = pltpu.get_barrier_semaphore()
    for shift in range(1, ways):
        pl.semaphore_signal(barrier, inc=1, device_id={"tp": lax.rem(t + shift, ways)}, device_id_type=MESH)
    for shift in range(1, parts):
        pl.semaphore_signal(barrier, inc=1, device_id={"grp": lax.rem(g + shift, parts)}, device_id_type=MESH)
    for direction in range(2):
        @pl.when(has_next(direction))
        def _():
            pl.semaphore_signal(
                barrier, inc=1, device_id={"sp": s + 1 if direction == 0 else s - 1}, device_id_type=MESH
            )
    for copy in locals_:
        copy.wait()
    neighbours = jnp.minimum(s, 1) + jnp.minimum(shards - 1 - s, 1)
    pl.semaphore_wait(barrier, ways - 1 + parts - 1 + neighbours)

    def tp_copy(ref, slot, sems, kind, shift):
        return pltpu.make_async_remote_copy(
            src_ref=ref.at[slot],
            dst_ref=ref.at[slot],
            send_sem=sems.at[kind, 0, shift - 1],
            recv_sem=sems.at[kind, 1, shift - 1],
            device_id={"tp": lax.rem(t + shift, ways)},
            device_id_type=MESH,
        )

    def tp_send(ref, sems, kind):
        for shift in range(1, ways):
            tp_copy(ref, t, sems, kind, shift).start()

    def tp_wait(ref, sems, kind):
        for shift in range(1, ways):
            tp_copy(ref, lax.rem(t + ways - shift, ways), sems, kind, shift).wait_recv()

    def gates_copy(block, index):
        return pltpu.make_async_remote_copy(
            src_ref=gates.at[block], dst_ref=gates.at[block],
            send_sem=gt_send.at[index], recv_sem=gt_recv.at[index],
            device_id={"sp": s + 1}, device_id_type=MESH,
        )

    def kv_copy(block, index):
        return pltpu.make_async_remote_copy(
            src_ref=kv.at[block], dst_ref=kv.at[block],
            send_sem=kv_send.at[index], recv_sem=kv_recv.at[index],
            device_id={"sp": s + 1}, device_id_type=MESH,
        )

    halo = pltpu.make_async_remote_copy(
        src_ref=wkv.at[pl.ds(rows, WINDOW), :], dst_ref=wkv.at[pl.ds(0, WINDOW), :],
        send_sem=halo_sem.at[0], recv_sem=halo_sem.at[1],
        device_id={"sp": s + 1}, device_id_type=MESH,
    )

    tp_send(tok, tok_sem, 0)
    send_own(0)
    send_own(1)

    @pl.when(has_next(0))
    def _():
        gates_copy(s, 0).start()

    tp_wait(tok, tok_sem, 0)
    share = depth // ways
    squares = jnp.zeros((rows, 1), jnp.float32)
    for way in range(ways):
        x = tok[way].astype(jnp.float32)
        squares = squares + jnp.sum(x * x, axis=-1, keepdims=True)
    scale = lax.rsqrt(squares * (1.0 / depth) + epsilon)
    for way in range(ways):
        at = slice(way * share, (way + 1) * share)
        normed[:, at] = (tok[way].astype(jnp.float32) * scale * norm_gain[:, at]).astype(jnp.bfloat16)

    @pl.loop(1, shards)
    def _(step):
        @pl.when(step == shards - 1)
        def _():
            send_own(2)

        relay(0, step)
        relay(1, step)

    def project(weight_ref, offset, width, flags, gain_at, store):
        raw = jnp.dot(normed[...], weight_ref[:, offset : offset + width], preferred_element_type=jnp.float32)
        for at in range(0, width, PAIR):
            part = raw[:, at : at + PAIR]
            first, second = flags[at // HEAD], flags[at // HEAD + 1]
            if first or second:
                power = part * part
                lower = jnp.sum(jnp.where(low, power, 0.0), axis=-1, keepdims=True)
                upper = jnp.sum(jnp.where(low, 0.0, power), axis=-1, keepdims=True)
                factor = jnp.where(
                    low,
                    lax.rsqrt(lower * (1.0 / HEAD) + epsilon),
                    lax.rsqrt(upper * (1.0 / HEAD) + epsilon),
                )
                scaled = part * factor * head_gain[:, gain_at + at : gain_at + at + PAIR]
                part = scaled if first and second else jnp.where(low if first else ~low, scaled, part)
            store(at, part.astype(jnp.bfloat16))

    def store_wkv(at, value):
        wkv[WINDOW : WINDOW + rows, at : at + PAIR] = value

    def store_kv(at, value):
        kv[s, :, at : at + PAIR] = value

    def store_q(at, value):
        queries[:, at : at + PAIR] = value * jnp.bfloat16(HEAD ** -0.5)

    small = 2 * groups * HEAD
    wait_mirror(0)
    project(w_kv, 2 * width, small, (True,) * groups + (False,) * groups, 2 * width, store_wkv)
    project(w_kv, 0, 2 * width, (True,) * heads + (False,) * heads, 0, store_kv)
    wait_mirror(1)
    project(w_q, 0, 2 * width, (True,) * (2 * heads), 2 * width + small, store_q)

    @pl.when(has_next(0))
    def _():
        halo.start()
        kv_copy(s, 0).start()

    @pl.when(s == 0)
    def _():
        wkv[0:WINDOW, :] = jnp.zeros((WINDOW, small), jnp.bfloat16)

    diagonal = lax.broadcasted_iota(jnp.int32, (rows, rows), 0) >= lax.broadcasted_iota(
        jnp.int32, (rows, rows), 1
    )

    def absorb(block, first):
        for head in range(heads):
            lanes = head // 2 * PAIR
            pick = low if head % 2 == 0 else ~low
            mine = jnp.where(pick, queries[:, width + lanes : width + lanes + PAIR], jnp.bfloat16(0))
            keys = kv[block, :, lanes : lanes + PAIR]
            values = kv[block, :, width + lanes : width + lanes + PAIR]
            scores = lax.dot_general(mine, keys, contract, preferred_element_type=jnp.float32)
            scores = scores - gates[block, head : head + 1, :]
            if first:
                scores = jnp.where(diagonal, scores, big_negative)
                top = jnp.max(scores, axis=-1, keepdims=True)
                weights = jnp.where(diagonal, jnp.exp(scores - top), 0.0)
            else:
                old = top_s[head, :, 0:1]
                top = jnp.maximum(old, jnp.max(scores, axis=-1, keepdims=True))
                weights = jnp.exp(scores - top)
            total = jnp.sum(weights, axis=-1, keepdims=True)
            mixed = jnp.dot(weights.astype(jnp.bfloat16), values, preferred_element_type=jnp.float32)
            if not first:
                shrink = jnp.exp(old - top)
                total = total + total_s[head, :, 0:1] * shrink
                mixed = mixed + mixed_s[head] * shrink
            top_s[head, :, 0:1] = top
            total_s[head, :, 0:1] = total
            mixed_s[head] = mixed

    absorb(s, True)

    @pl.when(s > 0)
    def _():
        halo.wait_recv()

    for pair in range(heads // 2):
        lanes = pair * PAIR
        keys = wkv[:, pair * HEAD : (pair + 1) * HEAD]
        values = wkv[:, groups * HEAD + pair * HEAD : groups * HEAD + (pair + 1) * HEAD]
        keys = jnp.concatenate([keys, keys], axis=1)
        values = jnp.concatenate([values, values], axis=1)
        row_at = lax.broadcasted_iota(jnp.int32, (WINDOW, 2 * WINDOW), 0)
        col_at = lax.broadcasted_iota(jnp.int32, (WINDOW, 2 * WINDOW), 1)
        inside = (col_at > row_at) & (col_at <= row_at + WINDOW)
        for at in range(0, rows, WINDOW):
            near_queries = queries[at : at + WINDOW, lanes : lanes + PAIR]
            near, near_values = keys[at : at + 2 * WINDOW], values[at : at + 2 * WINDOW]
            valid = inside & ((col_at >= WINDOW) | (s > 0)) if at == 0 else inside
            results = []
            for half in range(2):
                head = pair * 2 + half
                mine = jnp.where(low if half == 0 else ~low, near_queries, jnp.bfloat16(0))
                scores = lax.dot_general(mine, near, contract, preferred_element_type=jnp.float32)
                sink = sink_ref[:, head : head + 1]
                top = jnp.maximum(
                    jnp.max(jnp.where(valid, scores, big_negative), axis=-1, keepdims=True), sink
                )
                weights = jnp.where(valid, jnp.exp(scores - top), 0.0)
                total = jnp.sum(weights, axis=-1, keepdims=True) + jnp.exp(sink - top)
                probs = (weights / total).astype(jnp.bfloat16)
                results.append(jnp.dot(probs, near_values, preferred_element_type=jnp.float32))
            win[t, at : at + WINDOW, lanes : lanes + PAIR] = jnp.where(low, results[0], results[1]).astype(
                jnp.bfloat16
            )

    @pl.loop(1, shards + 2)
    def _(wave):
        @pl.when(wave == 1)
        def _():
            send_own(3)
            tp_send(win, head_sem, 0)

        @pl.when(wave == 2)
        def _():
            send_own(4)

        @pl.when(s >= wave)
        def _():
            gates_copy(s - wave, wave - 1).wait_recv()
            kv_copy(s - wave, wave - 1).wait_recv()

            @pl.when(has_next(0))
            def _():
                gates_copy(s - wave, wave).start()
                kv_copy(s - wave, wave).start()

        for offset in range(3):
            step = wave - offset

            @pl.when((step >= 1) & (step < shards))
            def _():
                relay(2 + offset, step)

        @pl.when(s >= wave)
        def _():
            absorb(s - wave, False)

        @pl.when(wave == FORGET_DONE(shards))
        def _():
            for pair in range(heads // 2):
                even, odd = 2 * pair, 2 * pair + 1
                mixed = jnp.where(
                    low, mixed_s[even] / total_s[even, :, 0:1], mixed_s[odd] / total_s[odd, :, 0:1]
                )
                forg[t, :, pair * PAIR : (pair + 1) * PAIR] = mixed.astype(jnp.bfloat16)
            tp_send(forg, head_sem, 1)

    wait_mirror(2)
    gate_s[0] = jax.nn.sigmoid(jnp.dot(normed[...], w_m0[...], preferred_element_type=jnp.float32))
    wait_mirror(3)
    gate_s[1] = jax.nn.sigmoid(jnp.dot(normed[...], w_m1[...], preferred_element_type=jnp.float32))
    tp_wait(win, head_sem, 0)
    tp_wait(forg, head_sem, 1)
    wait_mirror(4)
    total = None
    for branch, ref in enumerate((win, forg)):
        projection = None
        for way in range(ways):
            term = jnp.dot(
                ref[way], w_br[branch, way * width : (way + 1) * width, :], preferred_element_type=jnp.float32
            )
            projection = term if projection is None else projection + term
        gated = gate_s[branch] * projection
        total = gated if total is None else total + gated
    out_ref[...] = total.astype(jnp.bfloat16)

    for shift in range(1, ways):
        tp_copy(tok, t, tok_sem, 0, shift).wait_send()
        tp_copy(win, t, head_sem, 0, shift).wait_send()
        tp_copy(forg, t, head_sem, 1, shift).wait_send()

    @pl.when(has_next(0))
    def _():
        halo.wait_send()

    @pl.loop(0, shards)
    def _(step):
        @pl.when(has_next(0) & (s >= step))
        def _():
            kv_copy(s - step, step).wait_send()
            gates_copy(s - step, step).wait_send()

        for chunk in range(len(chunks)):
            for direction in range(2):
                @pl.when(has_next(direction) & has_source(direction, step))
                def _():
                    z_copy(direction, chunk, source(direction, step), step).wait_send()

                @pl.when((step >= 1) & has_source(direction, step))
                def _():
                    for shift in range(1, parts):
                        y_copy(direction, chunk, source(direction, step), step - 1, shift, g).wait_send()


def FORGET_DONE(shards):
    return max(shards - 1, 1)


def on_device(
    tokens,
    norm_gain,
    qk_gain,
    w_query_window,
    w_key_window,
    w_value_window,
    sink_logits,
    w_query_forget,
    w_key_forget,
    w_value_forget,
    gate_cum,
    w_merge,
    w_branch,
):
    rows, share = tokens.shape
    shards, parts, ways = lax.axis_size("sp"), lax.axis_size("grp"), lax.axis_size("tp")
    heads = w_query_window.shape[1] // HEAD
    groups = w_key_window.shape[1] // HEAD
    channels = w_merge.shape[2]
    depth, width, small = share * ways, heads * HEAD, 2 * groups * HEAD
    kv_in = jnp.concatenate([w_key_forget, w_value_forget, w_key_window, w_value_window], axis=1)
    q_in = jnp.concatenate([w_query_window, w_query_forget], axis=1)
    head_gains = jnp.concatenate(
        [
            jnp.tile(qk_gain[3], heads),
            jnp.ones((width,), jnp.float32),
            jnp.tile(qk_gain[1], groups),
            jnp.ones((groups * HEAD,), jnp.float32),
            jnp.tile(qk_gain[0], heads),
            jnp.tile(qk_gain[2], heads),
        ]
    )[None]
    half = jnp.bfloat16
    dma = pltpu.SemaphoreType.DMA
    anywhere, inside = pl.BlockSpec(memory_space=pl.ANY), pl.BlockSpec(memory_space=pltpu.VMEM)
    return pl.pallas_call(
        functools.partial(layer_kernel, heads, groups),
        out_shape=jax.ShapeDtypeStruct((rows, channels), half),
        in_specs=[anywhere] * 6 + [inside] * 3,
        out_specs=inside,
        scratch_shapes=[
            pltpu.VMEM((ways, rows, share), half),
            pltpu.VMEM((rows, depth), half),
            pltpu.VMEM((depth, 2 * width + small), half),
            pltpu.VMEM((depth, 2 * width), half),
            pltpu.VMEM((depth, channels), half),
            pltpu.VMEM((depth, channels), half),
            pltpu.VMEM((2, ways * width, channels), half),
            pltpu.VMEM((shards, rows, 2 * width), half),
            pltpu.VMEM((shards, heads, rows), jnp.float32),
            pltpu.VMEM((rows + WINDOW, small), half),
            pltpu.VMEM((rows, 2 * width), half),
            pltpu.VMEM((ways, rows, width), half),
            pltpu.VMEM((ways, rows, width), half),
            pltpu.VMEM((heads, rows, 128), jnp.float32),
            pltpu.VMEM((heads, rows, 128), jnp.float32),
            pltpu.VMEM((heads, rows, PAIR), jnp.float32),
            pltpu.VMEM((2, rows, channels), jnp.float32),
            dma((7,)),
            dma((1, 2, ways - 1)),
            dma((2, 5, shards)),
            dma((2, 5, shards)),
            dma((2, 5, shards, parts - 1)),
            dma((2, 5, shards, parts - 1)),
            dma((shards,)),
            dma((shards,)),
            dma((shards,)),
            dma((shards,)),
            dma((2,)),
            dma((2, 2, ways - 1)),
        ],
        compiler_params=pltpu.CompilerParams(
            collective_id=0, has_side_effects=True, vmem_limit_bytes=VMEM_LIMIT
        ),
        name="layer",
    )(
        tokens, kv_in, q_in, w_merge.reshape(w_merge.shape[0], -1), w_branch, gate_cum.T,
        norm_gain[None], head_gains, sink_logits[None],
    )


def solution(mesh):
    return jax.shard_map(
        on_device,
        mesh=mesh,
        in_specs=(
            P(("grp", "sp"), "tp"),
            P(),
            P(),
            P("sp", "tp"),
            P("sp", "tp"),
            P("sp", "tp"),
            P("tp"),
            P("sp", "tp"),
            P("sp", "tp"),
            P("sp", "tp"),
            P(("grp", "sp"), "tp"),
            P("sp", None, "tp"),
            P(None, "sp", "tp"),
        ),
        out_specs=P(("grp", "sp"), "tp"),
        check_vma=False,
    )
```

```python
import functools

import jax
import jax.numpy as jnp
from jax import lax
from jax.experimental import pallas as pl
from jax.experimental.pallas import tpu as pltpu
from jax.sharding import PartitionSpec as P

HEAD = 64
PAIR = 2 * HEAD
WINDOW = 128

epsilon = 1e-06
big_negative = -1e30
MESH = pl.DeviceIdType.MESH
VMEM_LIMIT = 60 * 1024 * 1024


def layer_kernel(
    heads, groups,
    tokens_in, qw_in, kvw_in, qf_in, kf_in, vf_in, merge_in, branch_in, gates_in, norm_gain, qk_gain, sink_ref,
    out_ref,
    tok, normed, w_kv, w_q, w_m0, w_m1, w_b0, w_b1, kv, gates, wkv, queries, win, forg, top_s, total_s, mixed_s, gate_s,
    local_sem, tok_sem, z_send, z_recv, y_send, y_recv, kv_send, kv_recv, gt_send, gt_recv, halo_sem, head_sem,
):
    shards, parts, ways = lax.axis_size("sp"), lax.axis_size("grp"), lax.axis_size("tp")
    s, g, t = lax.axis_index("sp"), lax.axis_index("grp"), lax.axis_index("tp")
    rows, depth = normed.shape
    width = heads * HEAD
    low = lax.broadcasted_iota(jnp.int32, (1, PAIR), 1) < HEAD
    contract = (((1,), (1,)), ((), ()))

    chunks = [w_kv, w_q, w_m0, w_m1, w_b0, w_b1]

    def view(chunk, block, part=None):
        ref = chunks[chunk]
        axis = ref.ndim - 2
        share = ref.shape[axis] // shards
        start, size = block * share, share
        if part is not None:
            size = share // parts
            start = start + part * size
        at = pl.ds(pl.multiple_of(start, size), size)
        return ref.at[at, :] if axis == 0 else ref.at[:, at, :]

    def z_copy(direction, chunk, block, index):
        return pltpu.make_async_remote_copy(
            src_ref=view(chunk, block, g),
            dst_ref=view(chunk, block, g),
            send_sem=z_send.at[direction, chunk, index],
            recv_sem=z_recv.at[direction, chunk, index],
            device_id={"sp": s + 1 if direction == 0 else s - 1},
            device_id_type=MESH,
        )

    def y_copy(direction, chunk, block, index, shift, part):
        return pltpu.make_async_remote_copy(
            src_ref=view(chunk, block, part),
            dst_ref=view(chunk, block, part),
            send_sem=y_send.at[direction, chunk, index, shift - 1],
            recv_sem=y_recv.at[direction, chunk, index, shift - 1],
            device_id={"grp": lax.rem(g + shift, parts)},
            device_id_type=MESH,
        )

    def has_next(direction):
        return s + 1 < shards if direction == 0 else s > 0

    def source(direction, step):
        return s - step if direction == 0 else s + step

    def has_source(direction, step):
        return s >= step if direction == 0 else s + step < shards

    def send_own(chunk):
        for direction in range(2):
            @pl.when(has_next(direction))
            def _():
                z_copy(direction, chunk, s, 0).start()

    def relay(chunk, step):
        for direction in range(2):
            @pl.when(has_source(direction, step))
            def _():
                block = source(direction, step)
                z_copy(direction, chunk, block, step - 1).wait_recv()

                @pl.when(has_next(direction) & (step < shards - 1))
                def _():
                    z_copy(direction, chunk, block, step).start()

                for shift in range(1, parts):
                    y_copy(direction, chunk, block, step - 1, shift, g).start()

    def wait_mirror(chunk):
        @pl.loop(1, shards)
        def _(step):
            for direction in range(2):
                @pl.when(has_source(direction, step))
                def _():
                    for shift in range(1, parts):
                        part = lax.rem(g + parts - shift, parts)
                        y_copy(direction, chunk, source(direction, step), step - 1, shift, part).wait_recv()

    def local(index, src, dst):
        return pltpu.make_async_copy(src, dst, local_sem.at[index])

    channels = out_ref.shape[1]
    small = 2 * groups * HEAD
    pieces = [
        (tokens_in, tok.at[t]),
        (gates_in, gates.at[s]),
        (merge_in.at[:, 0:channels], view(2, s)),
        (merge_in.at[:, channels : 2 * channels], view(3, s)),
        (branch_in.at[0], view(4, s)),
        (branch_in.at[1], view(5, s)),
    ]
    for chunk, arrays in ((0, (kf_in, vf_in, kvw_in)), (1, (qw_in, qf_in))):
        start = 0
        for array in arrays:
            size = array.shape[1]
            pieces.append((array, view(chunk, s).at[:, start : start + size]))
            start += size
    locals_ = [local(index, src, dst) for index, (src, dst) in enumerate(pieces)]
    for copy in locals_:
        copy.start()

    barrier = pltpu.get_barrier_semaphore()
    for shift in range(1, ways):
        pl.semaphore_signal(barrier, inc=1, device_id={"tp": lax.rem(t + shift, ways)}, device_id_type=MESH)
    for shift in range(1, parts):
        pl.semaphore_signal(barrier, inc=1, device_id={"grp": lax.rem(g + shift, parts)}, device_id_type=MESH)
    for direction in range(2):
        @pl.when(has_next(direction))
        def _():
            pl.semaphore_signal(
                barrier, inc=1, device_id={"sp": s + 1 if direction == 0 else s - 1}, device_id_type=MESH
            )
    for copy in locals_:
        copy.wait()
    neighbours = jnp.minimum(s, 1) + jnp.minimum(shards - 1 - s, 1)
    pl.semaphore_wait(barrier, ways - 1 + parts - 1 + neighbours)

    def tp_copy(ref, slot, sems, kind, shift):
        return pltpu.make_async_remote_copy(
            src_ref=ref.at[slot],
            dst_ref=ref.at[slot],
            send_sem=sems.at[kind, 0, shift - 1],
            recv_sem=sems.at[kind, 1, shift - 1],
            device_id={"tp": lax.rem(t + shift, ways)},
            device_id_type=MESH,
        )

    def tp_send(ref, sems, kind):
        for shift in range(1, ways):
            tp_copy(ref, t, sems, kind, shift).start()

    def tp_wait(ref, sems, kind):
        for shift in range(1, ways):
            tp_copy(ref, lax.rem(t + ways - shift, ways), sems, kind, shift).wait_recv()

    def gates_copy(block, index):
        return pltpu.make_async_remote_copy(
            src_ref=gates.at[block], dst_ref=gates.at[block],
            send_sem=gt_send.at[index], recv_sem=gt_recv.at[index],
            device_id={"sp": s + 1}, device_id_type=MESH,
        )

    def kv_copy(block, index):
        return pltpu.make_async_remote_copy(
            src_ref=kv.at[block], dst_ref=kv.at[block],
            send_sem=kv_send.at[index], recv_sem=kv_recv.at[index],
            device_id={"sp": s + 1}, device_id_type=MESH,
        )

    halo = pltpu.make_async_remote_copy(
        src_ref=wkv.at[pl.ds(rows, WINDOW), :], dst_ref=wkv.at[pl.ds(0, WINDOW), :],
        send_sem=halo_sem.at[0], recv_sem=halo_sem.at[1],
        device_id={"sp": s + 1}, device_id_type=MESH,
    )

    tp_send(tok, tok_sem, 0)
    send_own(0)
    send_own(1)

    @pl.when(has_next(0))
    def _():
        gates_copy(s, 0).start()

    @pl.loop(1, shards)
    def _(step):
        @pl.when(step == shards - 1)
        def _():
            send_own(2)
            tp_wait(tok, tok_sem, 0)
            share = depth // ways
            squares = jnp.zeros((rows, 1), jnp.float32)
            for way in range(ways):
                x = tok[way].astype(jnp.float32)
                squares = squares + jnp.sum(x * x, axis=-1, keepdims=True)
            scale = lax.rsqrt(squares * (1.0 / depth) + epsilon)
            for way in range(ways):
                at = slice(way * share, (way + 1) * share)
                normed[:, at] = (tok[way].astype(jnp.float32) * scale * norm_gain[:, at]).astype(jnp.bfloat16)

        relay(0, step)
        relay(1, step)

    def project(weight_ref, offset, width, flags, store):
        raw = jnp.dot(normed[...], weight_ref[:, offset : offset + width], preferred_element_type=jnp.float32)
        for at in range(0, width, PAIR):
            part = raw[:, at : at + PAIR]
            first, second = flags[at // HEAD], flags[at // HEAD + 1]
            if first is not None or second is not None:
                power = part * part
                lower = jnp.sum(jnp.where(low, power, 0.0), axis=-1, keepdims=True)
                upper = jnp.sum(jnp.where(low, 0.0, power), axis=-1, keepdims=True)
                factor = jnp.where(
                    low,
                    lax.rsqrt(lower * (1.0 / HEAD) + epsilon),
                    lax.rsqrt(upper * (1.0 / HEAD) + epsilon),
                )
                gain = jnp.concatenate([qk_gain[k : k + 1, :] for k in (first or 0, second or 0)], axis=1)
                scaled = part * factor * gain
                if first is None or second is None:
                    scaled = jnp.where(~low if first is None else low, scaled, part)
                part = scaled
            store(at, part.astype(jnp.bfloat16))

    def store_wkv(at, value):
        wkv[WINDOW : WINDOW + rows, at : at + PAIR] = value

    def store_kv(at, value):
        kv[s, :, at : at + PAIR] = value

    def store_q(at, value):
        queries[:, at : at + PAIR] = value * jnp.bfloat16(HEAD ** -0.5)

    wait_mirror(0)
    project(w_kv, 2 * width, small, (1,) * groups + (None,) * groups, store_wkv)
    project(w_kv, 0, 2 * width, (3,) * heads + (None,) * heads, store_kv)
    wait_mirror(1)
    project(w_q, 0, 2 * width, (0,) * heads + (2,) * heads, store_q)

    @pl.when(has_next(0))
    def _():
        halo.start()
        kv_copy(s, 0).start()

    @pl.when(s == 0)
    def _():
        wkv[0:WINDOW, :] = jnp.zeros((WINDOW, small), jnp.bfloat16)

    diagonal = lax.broadcasted_iota(jnp.int32, (rows, rows), 0) >= lax.broadcasted_iota(
        jnp.int32, (rows, rows), 1
    )

    def absorb(block, first):
        for head in range(heads):
            lanes = head // 2 * PAIR
            pick = low if head % 2 == 0 else ~low
            mine = jnp.where(pick, queries[:, width + lanes : width + lanes + PAIR], jnp.bfloat16(0))
            keys = kv[block, :, lanes : lanes + PAIR]
            values = kv[block, :, width + lanes : width + lanes + PAIR]
            scores = lax.dot_general(mine, keys, contract, preferred_element_type=jnp.float32)
            scores = scores - gates[block, head : head + 1, :]
            if first:
                scores = jnp.where(diagonal, scores, big_negative)
                top = jnp.max(scores, axis=-1, keepdims=True)
                weights = jnp.where(diagonal, jnp.exp(scores - top), 0.0)
            else:
                old = top_s[head, :, 0:1]
                top = jnp.maximum(old, jnp.max(scores, axis=-1, keepdims=True))
                weights = jnp.exp(scores - top)
            total = jnp.sum(weights, axis=-1, keepdims=True)
            mixed = jnp.dot(weights.astype(jnp.bfloat16), values, preferred_element_type=jnp.float32)
            if not first:
                shrink = jnp.exp(old - top)
                total = total + total_s[head, :, 0:1] * shrink
                mixed = mixed + mixed_s[head] * shrink
            top_s[head, :, 0:1] = top
            total_s[head, :, 0:1] = total
            mixed_s[head] = mixed

    absorb(s, True)

    @pl.when(s > 0)
    def _():
        halo.wait_recv()

    for pair in range(heads // 2):
        lanes = pair * PAIR
        keys = wkv[:, pair * HEAD : (pair + 1) * HEAD]
        values = wkv[:, groups * HEAD + pair * HEAD : groups * HEAD + (pair + 1) * HEAD]
        keys = jnp.concatenate([keys, keys], axis=1)
        values = jnp.concatenate([values, values], axis=1)
        row_at = lax.broadcasted_iota(jnp.int32, (WINDOW, 2 * WINDOW), 0)
        col_at = lax.broadcasted_iota(jnp.int32, (WINDOW, 2 * WINDOW), 1)
        inside = (col_at > row_at) & (col_at <= row_at + WINDOW)
        for at in range(0, rows, WINDOW):
            near_queries = queries[at : at + WINDOW, lanes : lanes + PAIR]
            near, near_values = keys[at : at + 2 * WINDOW], values[at : at + 2 * WINDOW]
            valid = inside & ((col_at >= WINDOW) | (s > 0)) if at == 0 else inside
            results = []
            for half in range(2):
                head = pair * 2 + half
                mine = jnp.where(low if half == 0 else ~low, near_queries, jnp.bfloat16(0))
                scores = lax.dot_general(mine, near, contract, preferred_element_type=jnp.float32)
                sink = sink_ref[:, head : head + 1]
                top = jnp.maximum(
                    jnp.max(jnp.where(valid, scores, big_negative), axis=-1, keepdims=True), sink
                )
                weights = jnp.where(valid, jnp.exp(scores - top), 0.0)
                total = jnp.sum(weights, axis=-1, keepdims=True) + jnp.exp(sink - top)
                probs = (weights / total).astype(jnp.bfloat16)
                results.append(jnp.dot(probs, near_values, preferred_element_type=jnp.float32))
            win[t, at : at + WINDOW, lanes : lanes + PAIR] = jnp.where(low, results[0], results[1]).astype(
                jnp.bfloat16
            )

    @pl.loop(1, shards + 3)
    def _(wave):
        @pl.when(wave == shards + 1)
        def _():
            wait_mirror(2)
            gate_s[0] = jax.nn.sigmoid(jnp.dot(normed[...], w_m0[...], preferred_element_type=jnp.float32))

        @pl.when(wave == 1)
        def _():
            send_own(3)
            tp_send(win, head_sem, 0)

        @pl.when(wave == 2)
        def _():
            send_own(4)
            send_own(5)

        @pl.when(s >= wave)
        def _():
            gates_copy(s - wave, wave - 1).wait_recv()
            kv_copy(s - wave, wave - 1).wait_recv()

            @pl.when(has_next(0))
            def _():
                gates_copy(s - wave, wave).start()
                kv_copy(s - wave, wave).start()

        for offset in range(4):
            step = wave - offset

            @pl.when((step >= 1) & (step < shards))
            def _():
                relay(2 + offset, step)

        @pl.when(s >= wave)
        def _():
            absorb(s - wave, False)

        @pl.when(wave == FORGET_DONE(shards))
        def _():
            for pair in range(heads // 2):
                even, odd = 2 * pair, 2 * pair + 1
                mixed = jnp.where(
                    low, mixed_s[even] / total_s[even, :, 0:1], mixed_s[odd] / total_s[odd, :, 0:1]
                )
                forg[t, :, pair * PAIR : (pair + 1) * PAIR] = mixed.astype(jnp.bfloat16)
            tp_send(forg, head_sem, 1)

    wait_mirror(3)
    gate_s[1] = jax.nn.sigmoid(jnp.dot(normed[...], w_m1[...], preferred_element_type=jnp.float32))
    tp_wait(win, head_sem, 0)
    tp_wait(forg, head_sem, 1)
    total = None
    for branch, (ref, w_out) in enumerate(((win, w_b0), (forg, w_b1))):
        wait_mirror(4 + branch)
        projection = None
        for way in range(ways):
            term = jnp.dot(
                ref[way], w_out[way * width : (way + 1) * width, :], preferred_element_type=jnp.float32
            )
            projection = term if projection is None else projection + term
        gated = gate_s[branch] * projection
        total = gated if total is None else total + gated
    out_ref[...] = total.astype(jnp.bfloat16)

    for shift in range(1, ways):
        tp_copy(tok, t, tok_sem, 0, shift).wait_send()
        tp_copy(win, t, head_sem, 0, shift).wait_send()
        tp_copy(forg, t, head_sem, 1, shift).wait_send()

    @pl.when(has_next(0))
    def _():
        halo.wait_send()

    @pl.loop(0, shards)
    def _(step):
        @pl.when(has_next(0) & (s >= step))
        def _():
            kv_copy(s - step, step).wait_send()
            gates_copy(s - step, step).wait_send()

        for chunk in range(len(chunks)):
            for direction in range(2):
                @pl.when(has_next(direction) & has_source(direction, step))
                def _():
                    z_copy(direction, chunk, source(direction, step), step).wait_send()

                @pl.when((step >= 1) & has_source(direction, step))
                def _():
                    for shift in range(1, parts):
                        y_copy(direction, chunk, source(direction, step), step - 1, shift, g).wait_send()


def FORGET_DONE(shards):
    return max(shards - 1, 1)


def on_device(
    tokens,
    norm_gain,
    qk_gain,
    w_query_window,
    w_key_window,
    w_value_window,
    sink_logits,
    w_query_forget,
    w_key_forget,
    w_value_forget,
    gate_cum,
    w_merge,
    w_branch,
):
    rows, share = tokens.shape
    shards, parts, ways = lax.axis_size("sp"), lax.axis_size("grp"), lax.axis_size("tp")
    heads = w_query_window.shape[1] // HEAD
    groups = w_key_window.shape[1] // HEAD
    channels = w_merge.shape[2]
    depth, width, small = share * ways, heads * HEAD, 2 * groups * HEAD
    half = jnp.bfloat16
    dma = pltpu.SemaphoreType.DMA
    anywhere, inside = pl.BlockSpec(memory_space=pl.ANY), pl.BlockSpec(memory_space=pltpu.VMEM)
    return pl.pallas_call(
        functools.partial(layer_kernel, heads, groups),
        out_shape=jax.ShapeDtypeStruct((rows, channels), half),
        in_specs=[anywhere] * 9 + [inside] * 3,
        out_specs=inside,
        scratch_shapes=[
            pltpu.VMEM((ways, rows, share), half),
            pltpu.VMEM((rows, depth), half),
            pltpu.VMEM((depth, 2 * width + small), half),
            pltpu.VMEM((depth, 2 * width), half),
            pltpu.VMEM((depth, channels), half),
            pltpu.VMEM((depth, channels), half),
            pltpu.VMEM((ways * width, channels), half),
            pltpu.VMEM((ways * width, channels), half),
            pltpu.VMEM((shards, rows, 2 * width), half),
            pltpu.VMEM((shards, heads, rows), jnp.float32),
            pltpu.VMEM((rows + WINDOW, small), half),
            pltpu.VMEM((rows, 2 * width), half),
            pltpu.VMEM((ways, rows, width), half),
            pltpu.VMEM((ways, rows, width), half),
            pltpu.VMEM((heads, rows, 128), jnp.float32),
            pltpu.VMEM((heads, rows, 128), jnp.float32),
            pltpu.VMEM((heads, rows, PAIR), jnp.float32),
            pltpu.VMEM((2, rows, channels), jnp.float32),
            dma((11,)),
            dma((1, 2, ways - 1)),
            dma((2, 6, shards)),
            dma((2, 6, shards)),
            dma((2, 6, shards, parts - 1)),
            dma((2, 6, shards, parts - 1)),
            dma((shards,)),
            dma((shards,)),
            dma((shards,)),
            dma((shards,)),
            dma((2,)),
            dma((2, 2, ways - 1)),
        ],
        compiler_params=pltpu.CompilerParams(
            collective_id=0, has_side_effects=True, vmem_limit_bytes=VMEM_LIMIT
        ),
        name="layer",
    )(
        tokens, w_query_window, jnp.concatenate([w_key_window, w_value_window], axis=1), w_query_forget, w_key_forget, w_value_forget,
        w_merge.reshape(w_merge.shape[0], -1), w_branch, gate_cum.T, norm_gain[None], qk_gain, sink_logits[None],
    )


def solution(mesh):
    return jax.shard_map(
        on_device,
        mesh=mesh,
        in_specs=(
            P(("grp", "sp"), "tp"),
            P(),
            P(),
            P("sp", "tp"),
            P("sp", "tp"),
            P("sp", "tp"),
            P("tp"),
            P("sp", "tp"),
            P("sp", "tp"),
            P("sp", "tp"),
            P(("grp", "sp"), "tp"),
            P("sp", None, "tp"),
            P(None, "sp", "tp"),
        ),
        out_specs=P(("grp", "sp"), "tp"),
        check_vma=False,
    )
```

```python
import functools

import jax
import jax.numpy as jnp
from jax import lax
from jax.experimental import pallas as pl
from jax.experimental.pallas import tpu as pltpu
from jax.sharding import PartitionSpec as P

HEAD = 64
PAIR = 2 * HEAD
WINDOW = 128

epsilon = 1e-06
big_negative = -1e30
MESH = pl.DeviceIdType.MESH
VMEM_LIMIT = 60 * 1024 * 1024


def layer_kernel(
    heads, groups,
    tokens_in, qw_in, kvw_in, qf_in, kf_in, vf_in, merge_in, branch_in, gates_in, norm_gain, qk_gain, sink_ref,
    out_ref,
    tok, normed, w_kv, w_q, w_m0, w_m1, w_b0, w_b1, kv, gates, wkv, queries, win, forg, top_s, total_s, mixed_s, gate_s,
    local_sem, tok_sem, z_send, z_recv, y_send, y_recv, kv_send, kv_recv, gt_send, gt_recv, halo_sem, head_sem,
):
    shards, parts, ways = lax.axis_size("sp"), lax.axis_size("grp"), lax.axis_size("tp")
    s, g, t = lax.axis_index("sp"), lax.axis_index("grp"), lax.axis_index("tp")
    rows, depth = normed.shape
    width = heads * HEAD
    low = lax.broadcasted_iota(jnp.int32, (1, PAIR), 1) < HEAD
    contract = (((1,), (1,)), ((), ()))

    chunks = [w_kv, w_q, w_m0, w_m1, w_b0, w_b1]

    def view(chunk, block, part=None):
        ref = chunks[chunk]
        axis = ref.ndim - 2
        share = ref.shape[axis] // shards
        start, size = block * share, share
        if part is not None:
            size = share // parts
            start = start + part * size
        at = pl.ds(pl.multiple_of(start, size), size)
        return ref.at[at, :] if axis == 0 else ref.at[:, at, :]

    def z_copy(direction, chunk, block, index):
        return pltpu.make_async_remote_copy(
            src_ref=view(chunk, block, g),
            dst_ref=view(chunk, block, g),
            send_sem=z_send.at[direction, chunk, index],
            recv_sem=z_recv.at[direction, chunk, index],
            device_id={"sp": s + 1 if direction == 0 else s - 1},
            device_id_type=MESH,
        )

    def y_copy(direction, chunk, block, index, shift, part):
        return pltpu.make_async_remote_copy(
            src_ref=view(chunk, block, part),
            dst_ref=view(chunk, block, part),
            send_sem=y_send.at[direction, chunk, index, shift - 1],
            recv_sem=y_recv.at[direction, chunk, index, shift - 1],
            device_id={"grp": lax.rem(g + shift, parts)},
            device_id_type=MESH,
        )

    def has_next(direction):
        return s + 1 < shards if direction == 0 else s > 0

    def source(direction, step):
        return s - step if direction == 0 else s + step

    def has_source(direction, step):
        return s >= step if direction == 0 else s + step < shards

    def send_own(chunk):
        for direction in range(2):
            @pl.when(has_next(direction))
            def _():
                z_copy(direction, chunk, s, 0).start()

    def relay(chunk, step):
        for direction in range(2):
            @pl.when(has_source(direction, step))
            def _():
                block = source(direction, step)
                z_copy(direction, chunk, block, step - 1).wait_recv()

                @pl.when(has_next(direction) & (step < shards - 1))
                def _():
                    z_copy(direction, chunk, block, step).start()

                for shift in range(1, parts):
                    y_copy(direction, chunk, block, step - 1, shift, g).start()

    def wait_mirror(chunk):
        @pl.loop(1, shards)
        def _(step):
            for direction in range(2):
                @pl.when(has_source(direction, step))
                def _():
                    for shift in range(1, parts):
                        part = lax.rem(g + parts - shift, parts)
                        y_copy(direction, chunk, source(direction, step), step - 1, shift, part).wait_recv()

    def local(index, src, dst):
        return pltpu.make_async_copy(src, dst, local_sem.at[index])

    channels = out_ref.shape[1]
    small = 2 * groups * HEAD
    pieces = [
        (tokens_in, tok.at[t]),
        (gates_in, gates.at[s]),
        (merge_in.at[:, 0:channels], view(2, s)),
        (merge_in.at[:, channels : 2 * channels], view(3, s)),
        (branch_in.at[0], view(4, s)),
        (branch_in.at[1], view(5, s)),
    ]
    for chunk, arrays in ((0, (kf_in, vf_in, kvw_in)), (1, (qw_in, qf_in))):
        start = 0
        for array in arrays:
            size = array.shape[1]
            pieces.append((array, view(chunk, s).at[:, start : start + size]))
            start += size
    locals_ = [local(index, src, dst) for index, (src, dst) in enumerate(pieces)]
    for copy in locals_:
        copy.start()

    barrier = pltpu.get_barrier_semaphore()
    for shift in range(1, ways):
        pl.semaphore_signal(barrier, inc=1, device_id={"tp": lax.rem(t + shift, ways)}, device_id_type=MESH)
    for shift in range(1, parts):
        pl.semaphore_signal(barrier, inc=1, device_id={"grp": lax.rem(g + shift, parts)}, device_id_type=MESH)
    for direction in range(2):
        @pl.when(has_next(direction))
        def _():
            pl.semaphore_signal(
                barrier, inc=1, device_id={"sp": s + 1 if direction == 0 else s - 1}, device_id_type=MESH
            )
    for copy in locals_:
        copy.wait()
    neighbours = jnp.minimum(s, 1) + jnp.minimum(shards - 1 - s, 1)
    pl.semaphore_wait(barrier, ways - 1 + parts - 1 + neighbours)

    def tp_copy(ref, slot, sems, kind, shift):
        return pltpu.make_async_remote_copy(
            src_ref=ref.at[slot],
            dst_ref=ref.at[slot],
            send_sem=sems.at[kind, 0, shift - 1],
            recv_sem=sems.at[kind, 1, shift - 1],
            device_id={"tp": lax.rem(t + shift, ways)},
            device_id_type=MESH,
        )

    def tp_send(ref, sems, kind):
        for shift in range(1, ways):
            tp_copy(ref, t, sems, kind, shift).start()

    def tp_wait(ref, sems, kind):
        for shift in range(1, ways):
            tp_copy(ref, lax.rem(t + ways - shift, ways), sems, kind, shift).wait_recv()

    def gates_copy(block, index):
        return pltpu.make_async_remote_copy(
            src_ref=gates.at[block], dst_ref=gates.at[block],
            send_sem=gt_send.at[index], recv_sem=gt_recv.at[index],
            device_id={"sp": s + 1}, device_id_type=MESH,
        )

    def kv_copy(block, index):
        return pltpu.make_async_remote_copy(
            src_ref=kv.at[block], dst_ref=kv.at[block],
            send_sem=kv_send.at[index], recv_sem=kv_recv.at[index],
            device_id={"sp": s + 1}, device_id_type=MESH,
        )

    halo = pltpu.make_async_remote_copy(
        src_ref=wkv.at[pl.ds(rows, WINDOW), :], dst_ref=wkv.at[pl.ds(0, WINDOW), :],
        send_sem=halo_sem.at[0], recv_sem=halo_sem.at[1],
        device_id={"sp": s + 1}, device_id_type=MESH,
    )

    tp_send(tok, tok_sem, 0)
    send_own(0)
    send_own(1)

    @pl.when(has_next(0))
    def _():
        gates_copy(s, 0).start()

    @pl.loop(1, shards)
    def _(step):
        @pl.when(step == shards - 1)
        def _():
            send_own(2)
            tp_wait(tok, tok_sem, 0)
            share = depth // ways
            squares = jnp.zeros((rows, 1), jnp.float32)
            for way in range(ways):
                x = tok[way].astype(jnp.float32)
                squares = squares + jnp.sum(x * x, axis=-1, keepdims=True)
            scale = lax.rsqrt(squares * (1.0 / depth) + epsilon)
            for way in range(ways):
                at = slice(way * share, (way + 1) * share)
                normed[:, at] = (tok[way].astype(jnp.float32) * scale * norm_gain[:, at]).astype(jnp.bfloat16)

        relay(0, step)
        relay(1, step)

    def project(weight_ref, offset, width, flags, store):
        raw = jnp.dot(normed[...], weight_ref[:, offset : offset + width], preferred_element_type=jnp.float32)
        for at in range(0, width, PAIR):
            part = raw[:, at : at + PAIR]
            first, second = flags[at // HEAD], flags[at // HEAD + 1]
            if first is not None or second is not None:
                power = part * part
                lower = jnp.sum(jnp.where(low, power, 0.0), axis=-1, keepdims=True)
                upper = jnp.sum(jnp.where(low, 0.0, power), axis=-1, keepdims=True)
                factor = jnp.where(
                    low,
                    lax.rsqrt(lower * (1.0 / HEAD) + epsilon),
                    lax.rsqrt(upper * (1.0 / HEAD) + epsilon),
                )
                gain = jnp.concatenate([qk_gain[k : k + 1, :] for k in (first or 0, second or 0)], axis=1)
                scaled = part * factor * gain
                if first is None or second is None:
                    scaled = jnp.where(~low if first is None else low, scaled, part)
                part = scaled
            store(at, part.astype(jnp.bfloat16))

    def store_wkv(at, value):
        wkv[WINDOW : WINDOW + rows, at : at + PAIR] = value

    def store_kv(at, value):
        kv[s, :, at : at + PAIR] = value

    def store_q(at, value):
        queries[:, at : at + PAIR] = value * jnp.bfloat16(HEAD ** -0.5)

    wait_mirror(0)
    project(w_kv, 2 * width, small, (1,) * groups + (None,) * groups, store_wkv)
    project(w_kv, 0, 2 * width, (3,) * heads + (None,) * heads, store_kv)
    wait_mirror(1)
    project(w_q, 0, 2 * width, (0,) * heads + (2,) * heads, store_q)

    @pl.when(has_next(0))
    def _():
        halo.start()
        kv_copy(s, 0).start()

    @pl.when(s == 0)
    def _():
        wkv[0:WINDOW, :] = jnp.zeros((WINDOW, small), jnp.bfloat16)

    diagonal = lax.broadcasted_iota(jnp.int32, (rows, rows), 0) >= lax.broadcasted_iota(
        jnp.int32, (rows, rows), 1
    )

    def absorb(block, first):
        for head in range(heads):
            lanes = head // 2 * PAIR
            pick = low if head % 2 == 0 else ~low
            mine = jnp.where(pick, queries[:, width + lanes : width + lanes + PAIR], jnp.bfloat16(0))
            keys = kv[block, :, lanes : lanes + PAIR]
            values = kv[block, :, width + lanes : width + lanes + PAIR]
            scores = lax.dot_general(mine, keys, contract, preferred_element_type=jnp.float32)
            scores = scores - gates[block, head : head + 1, :]
            if first:
                scores = jnp.where(diagonal, scores, big_negative)
                top = jnp.max(scores, axis=-1, keepdims=True)
                weights = jnp.where(diagonal, jnp.exp(scores - top), 0.0)
            else:
                old = top_s[head, :, 0:1]
                top = jnp.maximum(old, jnp.max(scores, axis=-1, keepdims=True))
                weights = jnp.exp(scores - top)
            total = jnp.sum(weights, axis=-1, keepdims=True)
            mixed = jnp.dot(weights.astype(jnp.bfloat16), values, preferred_element_type=jnp.float32)
            if not first:
                shrink = jnp.exp(old - top)
                total = total + total_s[head, :, 0:1] * shrink
                mixed = mixed + mixed_s[head] * shrink
            top_s[head, :, 0:1] = top
            total_s[head, :, 0:1] = total
            mixed_s[head] = mixed

    absorb(s, True)

    @pl.when(s > 0)
    def _():
        halo.wait_recv()

    for pair in range(heads // 2):
        lanes = pair * PAIR
        keys = wkv[:, pair * HEAD : (pair + 1) * HEAD]
        values = wkv[:, groups * HEAD + pair * HEAD : groups * HEAD + (pair + 1) * HEAD]
        keys = jnp.concatenate([keys, keys], axis=1)
        values = jnp.concatenate([values, values], axis=1)
        row_at = lax.broadcasted_iota(jnp.int32, (WINDOW, 2 * WINDOW), 0)
        col_at = lax.broadcasted_iota(jnp.int32, (WINDOW, 2 * WINDOW), 1)
        inside = (col_at > row_at) & (col_at <= row_at + WINDOW)
        for at in range(0, rows, WINDOW):
            near_queries = queries[at : at + WINDOW, lanes : lanes + PAIR]
            near, near_values = keys[at : at + 2 * WINDOW], values[at : at + 2 * WINDOW]
            valid = inside & ((col_at >= WINDOW) | (s > 0)) if at == 0 else inside
            results = []
            for half in range(2):
                head = pair * 2 + half
                mine = jnp.where(low if half == 0 else ~low, near_queries, jnp.bfloat16(0))
                scores = lax.dot_general(mine, near, contract, preferred_element_type=jnp.float32)
                sink = sink_ref[:, head : head + 1]
                top = jnp.maximum(
                    jnp.max(jnp.where(valid, scores, big_negative), axis=-1, keepdims=True), sink
                )
                weights = jnp.where(valid, jnp.exp(scores - top), 0.0)
                total = jnp.sum(weights, axis=-1, keepdims=True) + jnp.exp(sink - top)
                probs = (weights / total).astype(jnp.bfloat16)
                results.append(jnp.dot(probs, near_values, preferred_element_type=jnp.float32))
            win[t, at : at + WINDOW, lanes : lanes + PAIR] = jnp.where(low, results[0], results[1]).astype(
                jnp.bfloat16
            )

    @pl.loop(1, shards)
    def _(wave):
        @pl.when(wave == 1)
        def _():
            send_own(3)
            send_own(4)
            send_own(5)
            tp_send(win, head_sem, 0)

        @pl.when(s >= wave)
        def _():
            gates_copy(s - wave, wave - 1).wait_recv()
            kv_copy(s - wave, wave - 1).wait_recv()

            @pl.when(has_next(0))
            def _():
                gates_copy(s - wave, wave).start()
                kv_copy(s - wave, wave).start()

        @pl.when(s >= wave)
        def _():
            absorb(s - wave, False)

        @pl.when(wave == FORGET_DONE(shards))
        def _():
            for pair in range(heads // 2):
                even, odd = 2 * pair, 2 * pair + 1
                mixed = jnp.where(
                    low, mixed_s[even] / total_s[even, :, 0:1], mixed_s[odd] / total_s[odd, :, 0:1]
                )
                forg[t, :, pair * PAIR : (pair + 1) * PAIR] = mixed.astype(jnp.bfloat16)
            tp_send(forg, head_sem, 1)

        for chunk in range(2, len(chunks)):
            relay(chunk, wave)

    wait_mirror(2)
    gate_s[0] = jax.nn.sigmoid(jnp.dot(normed[...], w_m0[...], preferred_element_type=jnp.float32))
    wait_mirror(3)
    gate_s[1] = jax.nn.sigmoid(jnp.dot(normed[...], w_m1[...], preferred_element_type=jnp.float32))
    tp_wait(win, head_sem, 0)
    tp_wait(forg, head_sem, 1)
    total = None
    for branch, (ref, w_out) in enumerate(((win, w_b0), (forg, w_b1))):
        wait_mirror(4 + branch)
        projection = None
        for way in range(ways):
            term = jnp.dot(
                ref[way], w_out[way * width : (way + 1) * width, :], preferred_element_type=jnp.float32
            )
            projection = term if projection is None else projection + term
        gated = gate_s[branch] * projection
        total = gated if total is None else total + gated
    out_ref[...] = total.astype(jnp.bfloat16)

    for shift in range(1, ways):
        tp_copy(tok, t, tok_sem, 0, shift).wait_send()
        tp_copy(win, t, head_sem, 0, shift).wait_send()
        tp_copy(forg, t, head_sem, 1, shift).wait_send()

    @pl.when(has_next(0))
    def _():
        halo.wait_send()

    @pl.loop(0, shards)
    def _(step):
        @pl.when(has_next(0) & (s >= step))
        def _():
            kv_copy(s - step, step).wait_send()
            gates_copy(s - step, step).wait_send()

        for chunk in range(len(chunks)):
            for direction in range(2):
                @pl.when(has_next(direction) & has_source(direction, step))
                def _():
                    z_copy(direction, chunk, source(direction, step), step).wait_send()

                @pl.when((step >= 1) & has_source(direction, step))
                def _():
                    for shift in range(1, parts):
                        y_copy(direction, chunk, source(direction, step), step - 1, shift, g).wait_send()


def FORGET_DONE(shards):
    return max(shards - 1, 1)


def on_device(
    tokens,
    norm_gain,
    qk_gain,
    w_query_window,
    w_key_window,
    w_value_window,
    sink_logits,
    w_query_forget,
    w_key_forget,
    w_value_forget,
    gate_cum,
    w_merge,
    w_branch,
):
    rows, share = tokens.shape
    shards, parts, ways = lax.axis_size("sp"), lax.axis_size("grp"), lax.axis_size("tp")
    heads = w_query_window.shape[1] // HEAD
    groups = w_key_window.shape[1] // HEAD
    channels = w_merge.shape[2]
    depth, width, small = share * ways, heads * HEAD, 2 * groups * HEAD
    half = jnp.bfloat16
    dma = pltpu.SemaphoreType.DMA
    anywhere, inside = pl.BlockSpec(memory_space=pl.ANY), pl.BlockSpec(memory_space=pltpu.VMEM)
    return pl.pallas_call(
        functools.partial(layer_kernel, heads, groups),
        out_shape=jax.ShapeDtypeStruct((rows, channels), half),
        in_specs=[anywhere] * 9 + [inside] * 3,
        out_specs=inside,
        scratch_shapes=[
            pltpu.VMEM((ways, rows, share), half),
            pltpu.VMEM((rows, depth), half),
            pltpu.VMEM((depth, 2 * width + small), half),
            pltpu.VMEM((depth, 2 * width), half),
            pltpu.VMEM((depth, channels), half),
            pltpu.VMEM((depth, channels), half),
            pltpu.VMEM((ways * width, channels), half),
            pltpu.VMEM((ways * width, channels), half),
            pltpu.VMEM((shards, rows, 2 * width), half),
            pltpu.VMEM((shards, heads, rows), jnp.float32),
            pltpu.VMEM((rows + WINDOW, small), half),
            pltpu.VMEM((rows, 2 * width), half),
            pltpu.VMEM((ways, rows, width), half),
            pltpu.VMEM((ways, rows, width), half),
            pltpu.VMEM((heads, rows, 128), jnp.float32),
            pltpu.VMEM((heads, rows, 128), jnp.float32),
            pltpu.VMEM((heads, rows, PAIR), jnp.float32),
            pltpu.VMEM((2, rows, channels), jnp.float32),
            dma((11,)),
            dma((1, 2, ways - 1)),
            dma((2, 6, shards)),
            dma((2, 6, shards)),
            dma((2, 6, shards, parts - 1)),
            dma((2, 6, shards, parts - 1)),
            dma((shards,)),
            dma((shards,)),
            dma((shards,)),
            dma((shards,)),
            dma((2,)),
            dma((2, 2, ways - 1)),
        ],
        compiler_params=pltpu.CompilerParams(
            collective_id=0, has_side_effects=True, vmem_limit_bytes=VMEM_LIMIT
        ),
        name="layer",
    )(
        tokens, w_query_window, jnp.concatenate([w_key_window, w_value_window], axis=1), w_query_forget, w_key_forget, w_value_forget,
        w_merge.reshape(w_merge.shape[0], -1), w_branch, gate_cum.T, norm_gain[None], qk_gain, sink_logits[None],
    )


def solution(mesh):
    return jax.shard_map(
        on_device,
        mesh=mesh,
        in_specs=(
            P(("grp", "sp"), "tp"),
            P(),
            P(),
            P("sp", "tp"),
            P("sp", "tp"),
            P("sp", "tp"),
            P("tp"),
            P("sp", "tp"),
            P("sp", "tp"),
            P("sp", "tp"),
            P(("grp", "sp"), "tp"),
            P("sp", None, "tp"),
            P(None, "sp", "tp"),
        ),
        out_specs=P(("grp", "sp"), "tp"),
        check_vma=False,
    )
```
